32 devices in a mesh: kv: 16 (over z, y, x), tp: 2 (over core).
Axes of the slice: x: 2, y: 2, z: 4, core: 2. Of those that a mesh axis runs over, the one named last changes fastest.
Arguments:
- tokens: bfloat16 [32, 4096], P(None, 'kv'), may hold values from -12 to 12
- norm_gain: float32 [4096], P('kv'), may hold values from 0.1 to 1.9
- query_weight: bfloat16 [4096, 1024], P('kv', 'tp'), may hold values from -0.09375 to 0.09375
- key_weight: bfloat16 [4096, 1024], P('kv', 'tp'), may hold values from -0.09375 to 0.09375
- value_weight: bfloat16 [4096, 1024], P('kv', 'tp'), may hold values from -0.09375 to 0.09375
- forget_weight: bfloat16 [4096, 16], replicated, may hold values from -0.09375 to 0.09375
- forget_bias: float32 [16], replicated, may hold values from -4 to 4
- cache_keys: bfloat16 [32, 4096, 1024], P(None, 'kv', 'tp'), may hold values from -300 to 300
- cache_values: bfloat16 [32, 4096, 1024], P(None, 'kv', 'tp'), may hold values from -6 to 6
- cum_gate: float32 [32, 16, 4096], P(None, 'tp', 'kv'), may hold values from -4096 to 0, as said below
- lengths: int32 [32], replicated, may hold values from 1 to 4096, as said below
- out_weight: bfloat16 [1024, 4096], P('tp', 'kv'), may hold values from -0.75 to 0.75
- mlp_gain: float32 [4096], P('kv'), may hold values from 0.1 to 1.9
- up_weight: bfloat16 [4096, 16384], P('kv', 'tp'), may hold values from -0.09375 to 0.09375
- down_weight: bfloat16 [16384, 4096], P('tp', 'kv'), may hold values from -0.046875 to 0.046875
Outputs:
- layer_out: bfloat16 [32, 4096], P(None, 'kv')
The draws below stay inside these ranges and needn't reach their ends.
Inputs may be any that keep to these rules, and one draw needn't show every extreme that they name: The first lengths[b] cache positions of sequence b are live; some sequence has all 4096 positions live. `cum_gate`: never falls from one position to the next, and is 0 from position lengths[b] - 1 on.
All inputs are finite; a program needn't handle non-finite values.
Results may differ from the reference program's by a relative error of at most 0.017.
Values may be sent and summed in bfloat16 or wider, within the bound.
A program may use at most 128 MiB of HBM per device.

```python
import math
import jax
import jax.numpy as jnp
from jax import lax

D = 4096
FOCUS_CHANNELS = 16
HEAD = 64
FF = 16384
BATCH_STREAMS = 32
POS_DEV = 256
STORED_SLOTS = 4096
N_TP = 2


def shared_lengths(key):
    base_key = jax.random.fold_in(key, 41)
    unit = jax.random.randint(jax.random.fold_in(base_key, 1), (BATCH_STREAMS,), 1, STORED_SLOTS // 8 + 1, jnp.int32)
    power = jax.random.randint(jax.random.fold_in(base_key, 2), (BATCH_STREAMS,), 0, 4, jnp.int32)
    stretch = jnp.power(jnp.int32(2), power)
    lengths = jnp.minimum(unit * stretch, STORED_SLOTS)
    longest = jax.random.randint(jax.random.fold_in(base_key, 3), (), 0, BATCH_STREAMS, jnp.int32)
    return jnp.where(jnp.arange(BATCH_STREAMS, dtype=jnp.int32) == longest, STORED_SLOTS, lengths).astype(jnp.int32)


def draw_lengths(key, part):
    return shared_lengths(key)


def draw_tokens(key, part):
    token_key = jax.random.fold_in(key, 11)
    ramp = jnp.exp(jnp.linspace(math.log(0.5), math.log(2.5), D)).astype(jnp.float32)
    base = jax.random.normal(token_key, (BATCH_STREAMS, D), jnp.float32)
    row_scale = jnp.exp(jax.random.uniform(jax.random.fold_in(token_key, 3), (BATCH_STREAMS, 1), jnp.float32, -1.0, 1.0))
    return jnp.clip(base * ramp[None, :] * row_scale, -12.0, 12.0).astype(jnp.bfloat16)


def draw_cache_keys(key, part):
    keys_key = jax.random.fold_in(key, 21)
    base = jax.random.normal(keys_key, (BATCH_STREAMS, STORED_SLOTS, FOCUS_CHANNELS * HEAD), jnp.float32)
    lengths = shared_lengths(key)
    chosen_seq = jax.random.uniform(jax.random.fold_in(keys_key, 7), (BATCH_STREAMS,)) < 0.25
    first_seq = jax.random.randint(jax.random.fold_in(keys_key, 8), (), 0, BATCH_STREAMS, jnp.int32)
    chosen_seq = chosen_seq | (jnp.arange(BATCH_STREAMS, dtype=jnp.int32) == first_seq)
    spot_one = jax.random.randint(jax.random.fold_in(keys_key, 9), (BATCH_STREAMS,), 0, 1 << 30, jnp.int32) % lengths
    spot_two = jax.random.randint(jax.random.fold_in(keys_key, 10), (BATCH_STREAMS,), 0, 1 << 30, jnp.int32) % lengths
    slots = jnp.arange(STORED_SLOTS, dtype=jnp.int32)[None, :]
    spiked = ((slots == spot_one[:, None]) | (slots == spot_two[:, None])) & chosen_seq[:, None]
    power = jnp.full((BATCH_STREAMS, STORED_SLOTS), 120.0, jnp.float32)
    base = base * jnp.where(spiked, power, 1.0)[:, :, None]
    return jnp.clip(base, -300.0, 300.0).astype(jnp.bfloat16)


def draw_cum_gate(key, part):
    valve_seed_handle = jax.random.fold_in(key, 31)
    fast_share = 0.5
    fast = jax.random.uniform(jax.random.fold_in(valve_seed_handle, 1), (FOCUS_CHANNELS,)) < fast_share
    fast_rate = jax.random.uniform(jax.random.fold_in(valve_seed_handle, 2), (FOCUS_CHANNELS,), jnp.float32, 1.0 / 100, 1.0 / 30)
    slow_rate = jax.random.uniform(jax.random.fold_in(valve_seed_handle, 3), (FOCUS_CHANNELS,), jnp.float32, 0.5, 2.0) / STORED_SLOTS
    fading_speed = jnp.where(fast, fast_rate, slow_rate)
    blocks = STORED_SLOTS // POS_DEV
    tile_scaling = jnp.exp(jax.random.uniform(jax.random.fold_in(valve_seed_handle, 4), (BATCH_STREAMS, FOCUS_CHANNELS, blocks), jnp.float32, -0.7, 0.7))
    tile_scaling = jnp.repeat(tile_scaling, POS_DEV, axis=2)
    approximate_guess = jax.random.uniform(jax.random.fold_in(valve_seed_handle, 5), (BATCH_STREAMS, FOCUS_CHANNELS, STORED_SLOTS), jnp.float32, 0.3, 1.7)
    copy_volume = jax.random.uniform(jax.random.fold_in(valve_seed_handle, 6), (BATCH_STREAMS, FOCUS_CHANNELS, STORED_SLOTS)) < 3.0 / STORED_SLOTS
    storage_levels = jax.random.uniform(jax.random.fold_in(valve_seed_handle, 7), (BATCH_STREAMS, FOCUS_CHANNELS, STORED_SLOTS), jnp.float32, 0.22, 0.69)
    iteration_total = -fading_speed[None, :, None] * tile_scaling * approximate_guess - jnp.where(copy_volume, storage_levels, 0.0)
    after_all = jnp.cumsum(iteration_total[:, :, ::-1], axis=2)[:, :, ::-1] - iteration_total
    lengths = shared_lengths(key)
    last = jnp.broadcast_to((lengths - 1)[:, None, None], (BATCH_STREAMS, FOCUS_CHANNELS, 1)).astype(jnp.int32)
    at_end = jnp.take_along_axis(after_all, last, axis=2)
    after = after_all - at_end
    live = jnp.arange(STORED_SLOTS, dtype=jnp.int32)[None, None, :] < lengths[:, None, None]
    after = jnp.where(live, jnp.minimum(after, 0.0), 0.0)
    return jnp.maximum(after, -1.0 * STORED_SLOTS)


def level_of(key, dims, cuts, low, largest):
    gain, own = 1.0, jax.random.fold_in(key, 6)
    for dim, shards_of in cuts:
        steps = jnp.exp(jax.random.uniform(jax.random.fold_in(own, dim), (shards_of,), jnp.float32, low / len(cuts), largest / len(cuts)))
        gain = gain * jnp.repeat(steps, dims[dim] // shards_of).reshape([-1 if axis == dim else 1 for axis in range(len(dims))])
    return gain


def gaussian(own_key, shape, scale, most, split=(), held_as=jnp.bfloat16):
    gain = level_of(own_key, shape, split, -0.22, 0.18) if split else 1.0
    array = jax.random.normal(own_key, shape, jnp.float32) * scale * gain
    return jnp.minimum(jnp.maximum(array, -most), most).astype(held_as)


def setup_inputs(seed: int = 0) -> dict:
    streams_of = jax.random.split(jax.random.key(seed), 16)
    return {
        "tokens": draw_tokens(jax.random.fold_in(streams_of[15], 71), 0),
        "norm_gain": jnp.clip(1.0 + 0.18 * jax.random.normal(streams_of[1], (D,), jnp.float32), 0.1, 1.9),
        "query_weight": gaussian(streams_of[2], (D, FOCUS_CHANNELS * HEAD), D ** -0.5, 0.09375, ((0, 16), (1, 2))),
        "key_weight": gaussian(streams_of[3], (D, FOCUS_CHANNELS * HEAD), D ** -0.5, 0.09375, ((0, 16), (1, 2))),
        "value_weight": gaussian(streams_of[4], (D, FOCUS_CHANNELS * HEAD), D ** -0.5, 0.09375, ((0, 16), (1, 2))),
        "forget_weight": gaussian(streams_of[5], (D, FOCUS_CHANNELS), D ** -0.5, 0.09375),
        "forget_bias": gaussian(streams_of[6], (FOCUS_CHANNELS,), 1.0, 4.0, (), jnp.float32),
        "cache_keys": draw_cache_keys(jax.random.fold_in(streams_of[15], 71), 0),
        "cache_values": gaussian(streams_of[8], (BATCH_STREAMS, STORED_SLOTS, FOCUS_CHANNELS * HEAD), 1.0, 6.0, ((1, 16), (2, 2))),
        "cum_gate": draw_cum_gate(jax.random.fold_in(streams_of[15], 71), 0),
        "lengths": draw_lengths(jax.random.fold_in(streams_of[15], 71), 0),
        "out_weight": gaussian(streams_of[11], (FOCUS_CHANNELS * HEAD, D), (FOCUS_CHANNELS * HEAD // 16) ** -0.5, 0.75, ((0, 2), (1, 16))),
        "mlp_gain": jnp.clip(1.0 + 0.18 * jax.random.normal(streams_of[12], (D,), jnp.float32), 0.1, 1.9),
        "up_weight": gaussian(streams_of[13], (D, FF), D ** -0.5, 0.09375, ((0, 16), (1, 2))),
        "down_weight": gaussian(streams_of[14], (FF, D), FF ** -0.5, 0.046875, ((0, 2), (1, 16))),
    }


EPSILON = 1e-06

def attend_one(inputs):
    query, new_key, new_value, keys, values, gate, forget, length = inputs
    heads = gate.shape[0]
    blocks = gate.shape[1] // POS_DEV
    scale = HEAD ** (-0.5)
    query_f = query.astype(jnp.float32).reshape(heads, HEAD)
    keys_f = keys.astype(jnp.float32).reshape(keys.shape[0], heads, HEAD)
    values_f = values.astype(jnp.float32).reshape(blocks, POS_DEV, heads, HEAD)
    scores = jnp.einsum('hd,lhd->hl', query_f, keys_f) * scale + gate + forget[:, None]
    live = jnp.arange(keys.shape[0], dtype=jnp.int32)[None, :] < length
    scores = jnp.where(live, scores, -1e+30)
    own = lax.optimization_barrier(jnp.sum(query_f * new_key.astype(jnp.float32).reshape(heads, HEAD), axis=1)) * scale
    grouped = scores.reshape(heads, blocks, POS_DEV)
    live_blocks = live.reshape(1, blocks, POS_DEV)
    peak = lax.optimization_barrier(jnp.max(grouped, axis=2))
    top = jnp.maximum(lax.optimization_barrier(jnp.max(peak, axis=1)), own)
    local = jnp.where(live_blocks, jnp.exp(grouped - peak[:, :, None]), 0.0)
    shift = jnp.exp(peak - top[:, None])
    own_weight = jnp.exp(own - top)
    total = lax.optimization_barrier(jnp.sum(lax.optimization_barrier(jnp.sum(local, axis=2)) * shift, axis=1)) + own_weight
    local_b = lax.optimization_barrier(local.astype(jnp.bfloat16)).astype(jnp.float32)
    own_b = lax.optimization_barrier(own_weight.astype(jnp.bfloat16)).astype(jnp.float32)
    parts = jnp.einsum('hnp,nphd->hnd', local_b, values_f)
    numer = lax.optimization_barrier(jnp.sum(parts * shift[:, :, None], axis=1)) + own_b[:, None] * new_value.astype(jnp.float32).reshape(heads, HEAD)
    return (numer / total[:, None]).reshape(heads * HEAD)

def group_sum(left, right, groups):
    width = left.shape[1] // groups

    def one_group(index):
        part = lax.dynamic_slice_in_dim(left, index * width, width, 1)
        rows = lax.dynamic_slice_in_dim(right, index * width, width, 0)
        product = jnp.dot(part, rows, preferred_element_type=jnp.float32)
        return lax.optimization_barrier(product.astype(jnp.bfloat16)).astype(jnp.float32)
    return lax.optimization_barrier(jnp.sum(lax.map(one_group, jnp.arange(groups, dtype=jnp.int32)), axis=0))

def reference(tokens, norm_gain, query_weight, key_weight, value_weight, forget_weight, forget_bias, cache_keys, cache_values, cum_gate, lengths, out_weight, mlp_gain, up_weight, down_weight):
    tok_float = tokens.astype(jnp.float32)
    inv_rms = lax.rsqrt(lax.optimization_barrier(jnp.mean(tok_float * tok_float, axis=1, keepdims=True)) + EPSILON)
    normed = (tok_float * norm_gain).astype(jnp.bfloat16)
    query = (inv_rms * jnp.dot(normed, query_weight, preferred_element_type=jnp.float32)).astype(jnp.bfloat16)
    new_key = (inv_rms * jnp.dot(normed, key_weight, preferred_element_type=jnp.float32)).astype(jnp.bfloat16)
    new_value = (inv_rms * jnp.dot(normed, value_weight, preferred_element_type=jnp.float32)).astype(jnp.bfloat16)
    forget = jax.nn.log_sigmoid(inv_rms * jnp.dot(normed, forget_weight, preferred_element_type=jnp.float32) + forget_bias)
    attended = lax.map(attend_one, (query, new_key, new_value, cache_keys, cache_values, cum_gate, forget, lengths)).astype(jnp.bfloat16)
    mixed = group_sum(attended, out_weight, N_TP)
    hidden_in = (tok_float + mixed).astype(jnp.bfloat16)
    hidden_float = hidden_in.astype(jnp.float32)
    second_rms = lax.rsqrt(lax.optimization_barrier(jnp.mean(hidden_float * hidden_float, axis=1, keepdims=True)) + EPSILON)
    mlp_in = (hidden_float * mlp_gain).astype(jnp.bfloat16)
    up_total = jnp.dot(mlp_in, up_weight, preferred_element_type=jnp.float32)
    activated = jnp.square(jax.nn.relu(second_rms * up_total)).astype(jnp.bfloat16)
    down_total = group_sum(activated, down_weight, N_TP)
    return (hidden_float + down_total).astype(jnp.bfloat16)
```

```python
import functools

import jax
import jax.numpy as jnp
from jax import lax
from jax.experimental import pallas as pl
from jax.experimental.pallas import tpu as pltpu
from jax.sharding import PartitionSpec as P

HEAD = 64


EPSILON = 1e-06


def joined(part, axis, combine):
    gathered = jax.tree.map(lambda a: lax.all_gather(a, axis), part)

    def take(source):
        return jax.tree.map(lambda a: lax.dynamic_index_in_dim(a, source, 0, False), gathered)

    return lax.fori_loop(
        1, lax.axis_size(axis), lambda source, state: combine(state, take(source)), take(0)
    )


def weighted_merge(first, second):
    peak_a, total_a, accum_a = first
    peak_b, total_b, accum_b = second
    peak = jnp.maximum(peak_a, peak_b)
    factor_a = jnp.exp(peak_a - peak)
    factor_b = jnp.exp(peak_b - peak)
    accum = accum_a * jnp.repeat(factor_a, HEAD, axis=1) + accum_b * jnp.repeat(
        factor_b, HEAD, axis=1
    )
    return (peak, total_a * factor_a + total_b * factor_b, accum)


def shards(
    tokens,
    norm_gain,
    query_weight,
    key_weight,
    value_weight,
    forget_weight,
    forget_bias,
    cache_keys,
    cache_values,
    cum_gate,
    lengths,
    out_weight,
    mlp_gain,
    up_weight,
    down_weight,
):
    kv_rank = lax.axis_index("kv")
    tp_rank = lax.axis_index("tp")
    kv_count = lax.axis_size("kv")
    seqs_here, own_cols = tokens.shape
    model_width = own_cols * kv_count
    head_cols = query_weight.shape[1]
    heads_here = head_cols // HEAD
    span = cache_keys.shape[1]
    scale = HEAD ** (-0.5)
    tok_float = tokens.astype(jnp.float32)
    normed = (tok_float * norm_gain).astype(jnp.bfloat16)
    forget_rows = lax.dynamic_slice_in_dim(forget_weight, kv_rank * own_cols, own_cols, 0)
    squares, query_sum, key_sum, value_sum, forget_sum = lax.psum(
        (
            jnp.sum(tok_float * tok_float, axis=1),
            jnp.dot(normed, query_weight, preferred_element_type=jnp.float32),
            jnp.dot(normed, key_weight, preferred_element_type=jnp.float32),
            jnp.dot(normed, value_weight, preferred_element_type=jnp.float32),
            jnp.dot(normed, forget_rows, preferred_element_type=jnp.float32),
        ),
        "kv",
    )
    inv_rms = lax.rsqrt(squares / model_width + EPSILON)[:, None]
    query = (inv_rms * query_sum).astype(jnp.bfloat16)
    new_key = (inv_rms * key_sum).astype(jnp.bfloat16)
    new_value = (inv_rms * value_sum).astype(jnp.bfloat16)
    forget_all = jax.nn.log_sigmoid(inv_rms * forget_sum + forget_bias)
    forget_here = lax.dynamic_slice_in_dim(forget_all, tp_rank * heads_here, heads_here, 1)
    query_heads = query.reshape(seqs_here, heads_here, HEAD)
    key_heads = cache_keys.reshape(seqs_here, span, heads_here, HEAD)
    value_heads = cache_values.reshape(seqs_here, span, heads_here, HEAD)
    scores = (
        jnp.einsum("bhd,bphd->bhp", query_heads, key_heads, preferred_element_type=jnp.float32)
        * scale
    )
    scores = scores + cum_gate + forget_here[:, :, None]
    positions = kv_rank * span + lax.iota(jnp.int32, span)
    live = positions[None, None, :] < lengths[:, None, None]
    scores = jnp.where(live, scores, -1e30)
    peak = jnp.max(scores, axis=2)
    weights = jnp.where(live, jnp.exp(scores - peak[:, :, None]), 0.0)
    total = jnp.sum(weights, axis=2)
    accum = jnp.einsum(
        "bhp,bphd->bhd",
        weights.astype(jnp.bfloat16),
        value_heads,
        preferred_element_type=jnp.float32,
    ).reshape(seqs_here, head_cols)
    peak, total, accum = joined((peak, total, accum), "kv", weighted_merge)
    own_score = (
        jnp.sum(
            query_heads.astype(jnp.float32)
            * new_key.reshape(seqs_here, heads_here, HEAD).astype(jnp.float32),
            axis=2,
        )
        * scale
    )
    top = jnp.maximum(peak, own_score)
    cache_factor = jnp.exp(peak - top)
    own_weight = jnp.exp(own_score - top)
    denom = total * cache_factor + own_weight
    own_rounded = own_weight.astype(jnp.bfloat16).astype(jnp.float32)
    numer = accum.reshape(seqs_here, heads_here, HEAD) * cache_factor[:, :, None]
    numer = numer + own_rounded[:, :, None] * new_value.reshape(seqs_here, heads_here, HEAD).astype(
        jnp.float32
    )
    attended = (numer / denom[:, :, None]).reshape(seqs_here, head_cols).astype(jnp.bfloat16)
    mixed = lax.psum(
        jnp.dot(attended, out_weight, preferred_element_type=jnp.float32).astype(jnp.bfloat16), "tp"
    ).astype(jnp.float32)
    hidden_in = (tok_float + mixed).astype(jnp.bfloat16)
    hidden_float = hidden_in.astype(jnp.float32)
    mlp_in = (hidden_float * mlp_gain).astype(jnp.bfloat16)
    up_part = jnp.dot(mlp_in, up_weight, preferred_element_type=jnp.float32)
    hidden_squares = jnp.sum(hidden_float * hidden_float, axis=1)
    second_sq, up_total = lax.psum((hidden_squares, up_part), "kv")
    second_rms = lax.rsqrt(second_sq / model_width + EPSILON)[:, None]
    activated = jnp.square(jax.nn.relu(second_rms * up_total)).astype(jnp.bfloat16)
    down_part = jnp.dot(activated, down_weight, preferred_element_type=jnp.float32)
    down_total = lax.psum(down_part.astype(jnp.bfloat16), "tp").astype(jnp.float32)
    return (hidden_float + down_total).astype(jnp.bfloat16)


LANES = 128
NEG = -1e30
MESH = pl.DeviceIdType.MESH
F32 = jnp.float32
BF16 = jnp.bfloat16
QKV_SUM, QUERY_ALL, CACHE_SUM, ATT_ALL, MIX_PAIR, UP_SUM, SQ_ALL, ACT_ALL, DOWN_PAIR = range(9)


def lane_pick(x, lane, index):
    return jnp.sum(jnp.where(lane == index, x, 0.0), axis=-1, keepdims=True)


def step_kernel(n, nt, dims, *refs):
    rows, cols, heads, span, hidden, width = dims
    own = rows // n
    head_cols = heads * HEAD
    chunk = hidden // n
    len_ref = refs[0]
    sources = refs[1:15]
    out_ref = refs[15]
    held = refs[16:30]
    (extra, a_send, a_recv, q_own, q_all, c_send, c_recv, t_own, t_all, att, x_own, x_all,
     d_send, d_recv, s_own, s_all, g_own, g_all, y_own, y_all,
     lsem, ssem, rsem, psend, precv) = refs[30:]
    tok, ng, wq, wk, wv, fw, fb, ck, cv, cg, ow, mg, uw, dw = held
    me = lax.axis_index("kv")
    tp = lax.axis_index("tp")

    local = []
    for i, (source, target) in enumerate(zip(sources, held)):
        if i == 5:
            source = source.at[pl.ds(pl.multiple_of(me * cols, cols), cols), :]
        local.append(pltpu.make_async_copy(source, target, lsem.at[i]))
    for i in range(7):
        local[i].start()

    barrier = pltpu.get_barrier_semaphore()

    def greet(t, carry):
        pl.semaphore_signal(
            barrier, inc=1, device_id={"kv": lax.rem(me + t, n)}, device_id_type=MESH
        )
        return carry

    lax.fori_loop(1, n, greet, 0)
    for t in range(1, nt):
        pl.semaphore_signal(
            barrier, inc=1, device_id={"tp": lax.rem(tp + t, nt)}, device_id_type=MESH
        )
    for i in (7, 9, 8, 11, 10, 12, 13):
        local[i].start()

    def remote(phase, source, target, peer, slot):
        return pltpu.make_async_remote_copy(
            src_ref=source, dst_ref=target.at[slot], send_sem=ssem.at[phase, peer],
            recv_sem=rsem.at[phase, slot], device_id={"kv": peer}, device_id_type=MESH,
        )

    def send_to(phase, source_of, target, t):
        peer = lax.rem(me + t, n)
        remote(phase, source_of(peer), target, peer, me).start()

    def send_all(phase, source_of, target):
        def step(t, carry):
            send_to(phase, source_of, target, t)
            return carry

        lax.fori_loop(1, n, step, 0)

    def wait_from(phase, source_of, target, t):
        peer = lax.rem(me + n - t, n)
        remote(phase, source_of(peer), target, peer, peer).wait_recv()
        return peer

    def wait_all(phase, source_of, target):
        def step(t, carry):
            wait_from(phase, source_of, target, t)
            return carry

        lax.fori_loop(1, n, step, 0)

    def sent_all(phase, source_of, target):
        def step(t, carry):
            peer = lax.rem(me + t, n)
            remote(phase, source_of(peer), target, peer, me).wait_send()
            return carry

        lax.fori_loop(1, n, step, 0)

    def pair(index, source, target, t):
        peer = lax.rem(tp + t, nt)
        return pltpu.make_async_remote_copy(
            src_ref=source, dst_ref=target.at[tp], send_sem=psend.at[index, peer],
            recv_sem=precv.at[index, tp], device_id={"tp": peer}, device_id_type=MESH,
        )

    def pair_in(index, source, target, t):
        peer = lax.rem(tp + t, nt)
        return pltpu.make_async_remote_copy(
            src_ref=source, dst_ref=target.at[peer], send_sem=psend.at[index, peer],
            recv_sem=precv.at[index, peer], device_id={"tp": peer}, device_id_type=MESH,
        )

    lane = lax.broadcasted_iota(jnp.int32, (heads, LANES), 1)
    head = lax.broadcasted_iota(jnp.int32, (heads, LANES), 0)
    wide_lane = lax.broadcasted_iota(jnp.int32, (heads, head_cols), 1)
    wide_head = lax.broadcasted_iota(jnp.int32, (heads, head_cols), 0)
    mine = (wide_lane >= wide_head * HEAD) & (wide_lane < (wide_head + 1) * HEAD)

    def fold(x):
        x = jnp.where(mine, x, 0.0)
        total = x[:, :LANES]
        for k in range(1, head_cols // LANES):
            total = total + x[:, k * LANES:(k + 1) * LANES]
        return total + pltpu.roll(total, HEAD, axis=1)

    def spread(row):
        return fold(jnp.broadcast_to(row, (heads, head_cols)))

    def unfold(x):
        wide = jnp.concatenate([x] * (head_cols // LANES), axis=1)
        return jnp.sum(jnp.where(mine, wide, 0.0), axis=0, keepdims=True)

    for i in range(7):
        local[i].wait()
    tok_float = tok[...].astype(F32)
    normed = (tok_float * ng[...]).astype(BF16)
    extra[...] = jnp.zeros_like(extra)
    n_forget = fw.shape[1]
    extra[:, :n_forget] = jnp.dot(normed, fw[...], preferred_element_type=F32)
    extra[:, n_forget:n_forget + 1] = jnp.sum(tok_float * tok_float, axis=1, keepdims=True)
    for k, (w, at) in enumerate(((wq, 0), (wk, head_cols), (wv, 2 * head_cols), (None, 3 * head_cols))):
        if w is None:
            value, size = extra[...], LANES
        else:
            value, size = jnp.dot(normed, w[...], preferred_element_type=F32), head_cols
        for j in range(n):
            a_send[j, :, at:at + size] = value[j * own:(j + 1) * own, :]
    a_recv[me] = a_send[me]
    pl.semaphore_wait(barrier, n - 1 + nt - 1)
    part = lambda peer: a_send.at[peer]
    send_all(QKV_SUM, part, a_recv)
    wait_all(QKV_SUM, part, a_recv)
    total = jnp.sum(a_recv[...], axis=0)
    tail_lane = lax.broadcasted_iota(jnp.int32, (own, LANES), 1)
    tail = total[:, 3 * head_cols:]
    inv_rms = lax.rsqrt(lane_pick(tail, tail_lane, n_forget) / width + EPSILON)
    query = (inv_rms * total[:, :head_cols]).astype(BF16).astype(F32) * HEAD ** (-0.5)
    new_key = (inv_rms * total[:, head_cols:2 * head_cols]).astype(BF16).astype(F32)
    new_value = (inv_rms * total[:, 2 * head_cols:3 * head_cols]).astype(BF16).astype(F32)
    gate_in = inv_rms * tail
    q_own[...] = query
    q_all[me] = query
    q_src = lambda peer: q_own
    send_all(QUERY_ALL, q_src, q_all)

    own_terms = []
    for r in range(own):
        qf, kf, vf = (spread(x[r:r + 1, :]) for x in (query, new_key, new_value))
        score = jnp.sum(qf * kf, axis=1, keepdims=True) * 0.5
        raw = jnp.broadcast_to(gate_in[r:r + 1, :], (heads, LANES))
        raw = lane_pick(raw, lane, head + tp * heads)
        small_lane = lax.broadcasted_iota(jnp.int32, (heads, n_forget), 1)
        small_head = lax.broadcasted_iota(jnp.int32, (heads, n_forget), 0)
        bias = lane_pick(
            jnp.broadcast_to(fb[...], (heads, n_forget)), small_lane, small_head + tp * heads
        )
        z = raw + bias
        forget = jnp.minimum(z, 0.0) - jnp.log1p(jnp.exp(-jnp.abs(z)))
        own_terms.append((score, forget, vf))

    wait_all(QUERY_ALL, q_src, q_all)
    for i in (7, 9, 8):
        local[i].wait()
    place = me * span + lax.broadcasted_iota(jnp.int32, (heads, span), 1)
    group = 4 if n % 4 == 0 else 1

    def attend(g, carry):
        scores = []
        seqs = [(g * group + u, r) for u in range(group) for r in range(own)]
        for i, r in seqs:
            b = i * own + r
            row = jnp.broadcast_to(q_all[i, r:r + 1, :], (heads, head_cols))
            blocks = jnp.where(mine, row, 0.0).astype(BF16)
            s = lax.dot_general(
                blocks, ck[b], (((1,), (1,)), ((), ())), preferred_element_type=F32
            )
            scores.append(jnp.where(place < len_ref[b], s + cg[b], NEG))
        peaks = [jnp.max(s, axis=1, keepdims=True) for s in scores]
        weights = [
            jnp.where(s > 0.1 * NEG, jnp.exp(s - peak), 0.0) for s, peak in zip(scores, peaks)
        ]
        totals = [jnp.sum(w, axis=1, keepdims=True) for w in weights]
        for (i, r), w, peak, tot in zip(seqs, weights, peaks, totals):
            acc = fold(jnp.dot(w.astype(BF16), cv[i * own + r], preferred_element_type=F32))
            acc = jnp.where(lane == HEAD, peak, acc)
            c_send[i, r] = jnp.where(lane == HEAD + 1, tot, acc)
        return carry

    lax.fori_loop(0, n // group, attend, 0)
    c_recv[me] = c_send[me]
    c_src = lambda peer: c_send.at[peer]
    send_all(CACHE_SUM, c_src, c_recv)
    wait_all(CACHE_SUM, c_src, c_recv)
    for r in range(own):
        score, forget, vf = own_terms[r]
        parts = c_recv[:, r]
        peak = lane_pick(parts, lane[None], HEAD) + forget[None]
        top = jnp.maximum(jnp.max(peak, axis=0), score)
        merged = jnp.sum(parts * jnp.exp(peak - top[None]), axis=0)
        own_weight = jnp.exp(score - top)
        denom = lane_pick(merged, lane, HEAD + 1) + own_weight
        numer = merged + own_weight.astype(BF16).astype(F32) * vf
        done = jnp.where(lane < HEAD, numer / denom, 0.0).astype(BF16).astype(F32)
        t_own[r:r + 1, :] = unfold(done + pltpu.roll(done, HEAD, axis=1))
    t_all[me] = t_own[...]
    t_src = lambda peer: t_own
    send_all(ATT_ALL, t_src, t_all)
    wait_all(ATT_ALL, t_src, t_all)
    for j in range(n):
        att[j * own:(j + 1) * own, :] = t_all[j]
    for i in (10, 11, 12, 13):
        local[i].wait()
    mixed = jnp.dot(att[...].astype(BF16), ow[...], preferred_element_type=F32).astype(BF16)
    x_own[...] = mixed
    x_all[tp] = mixed
    for t in range(1, nt):
        pair(0, x_own, x_all, t).start()
    for t in range(1, nt):
        pair_in(0, x_own, x_all, t).wait_recv()
    hidden_in = (tok_float + jnp.sum(x_all[...].astype(F32), axis=0)).astype(BF16)
    hidden_float = hidden_in.astype(F32)
    mlp_in = (hidden_float * mg[...]).astype(BF16)

    sq_lane = lax.broadcasted_iota(jnp.int32, (rows, LANES), 1)
    sq_row = lax.broadcasted_iota(jnp.int32, (rows, LANES), 0)
    squares = jnp.sum(hidden_float * hidden_float, axis=1, keepdims=True)
    squares = jnp.sum(jnp.where(sq_lane == sq_row, squares, 0.0), axis=0, keepdims=True)
    s_own[...] = squares
    s_all[me] = squares
    s_src = lambda peer: s_own
    send_all(SQ_ALL, s_src, s_all)
    d_src = lambda peer: d_send.at[peer]

    def up(j):
        w = uw[:, pl.ds(pl.multiple_of(j * chunk, chunk), chunk)]
        return jnp.dot(mlp_in, w, preferred_element_type=F32)

    def up_step(t, carry):
        peer = lax.rem(me + t, n)
        d_send[peer] = up(peer).astype(BF16)
        send_to(UP_SUM, d_src, d_recv, t)
        return carry

    lax.fori_loop(1, n, up_step, 0)
    own_up = up(me)
    wait_all(SQ_ALL, s_src, s_all)
    second = jnp.broadcast_to(jnp.sum(s_all[...], axis=0), (rows, LANES))
    second_rms = lax.rsqrt(lane_pick(second, sq_lane, sq_row) / width + EPSILON)

    def up_take(t, acc):
        peer = wait_from(UP_SUM, d_src, d_recv, t)
        return acc + d_recv[peer].astype(F32)

    up_total = lax.fori_loop(1, n, up_take, own_up)
    activated = jnp.square(jnp.maximum(second_rms * up_total, 0.0)).astype(BF16)
    g_own[...] = activated
    g_src = lambda peer: g_own
    send_all(ACT_ALL, g_src, g_all)

    def down(value, j):
        w = dw[pl.ds(pl.multiple_of(j * chunk, chunk), chunk), :]
        return jnp.dot(value, w, preferred_element_type=F32)

    def down_step(t, acc):
        peer = wait_from(ACT_ALL, g_src, g_all, t)
        return acc + down(g_all[peer], peer)

    part_out = lax.fori_loop(1, n, down_step, down(activated, me)).astype(BF16)
    y_own[...] = part_out
    y_all[tp] = part_out
    for t in range(1, nt):
        pair(1, y_own, y_all, t).start()
    for t in range(1, nt):
        pair_in(1, y_own, y_all, t).wait_recv()
    out_ref[...] = (hidden_float + jnp.sum(y_all[...].astype(F32), axis=0)).astype(BF16)

    for phase, source_of, target in (
        (QKV_SUM, part, a_recv), (QUERY_ALL, q_src, q_all), (CACHE_SUM, c_src, c_recv),
        (ATT_ALL, t_src, t_all), (SQ_ALL, s_src, s_all), (UP_SUM, d_src, d_recv),
        (ACT_ALL, g_src, g_all),
    ):
        sent_all(phase, source_of, target)
    for t in range(1, nt):
        pair(0, x_own, x_all, t).wait_send()
        pair(1, y_own, y_all, t).wait_send()


def fits(n, rows, cols, heads, span, hidden):
    return (
        rows % n == 0 and rows <= LANES and cols % LANES == 0 and heads == 8
        and (heads * HEAD) % LANES == 0 and span % LANES == 0 and hidden % (n * LANES) == 0
    )


def fused(tokens, norm_gain, query_weight, key_weight, value_weight, forget_weight, forget_bias,
          cache_keys, cache_values, cum_gate, lengths, out_weight, mlp_gain, up_weight, down_weight):
    n, nt = lax.axis_size("kv"), lax.axis_size("tp")
    rows, cols = tokens.shape
    heads, span = cum_gate.shape[1:]
    hidden = up_weight.shape[1]
    head_cols = heads * HEAD
    own, chunk = rows // n, hidden // n
    ops = [
        tokens, norm_gain[None], query_weight, key_weight, value_weight, forget_weight,
        forget_bias[None], cache_keys, cache_values, cum_gate, out_weight, mlp_gain[None],
        up_weight, down_weight,
    ]
    shapes = [op.shape for op in ops]
    shapes[5] = (cols, forget_weight.shape[1])
    vm = pltpu.VMEM
    scratch = [vm(shape, op.dtype) for shape, op in zip(shapes, ops)] + [
        vm((rows, LANES), F32),
        vm((n, own, 3 * head_cols + LANES), F32),
        vm((n, own, 3 * head_cols + LANES), F32),
        vm((own, head_cols), F32),
        vm((n, own, head_cols), F32),
        vm((n, own, heads, LANES), F32),
        vm((n, own, heads, LANES), F32),
        vm((own, head_cols), F32),
        vm((n, own, head_cols), F32),
        vm((rows, head_cols), F32),
        vm((rows, cols), BF16),
        vm((nt, rows, cols), BF16),
        vm((n, rows, chunk), BF16),
        vm((n, rows, chunk), BF16),
        vm((1, LANES), F32),
        vm((n, 1, LANES), F32),
        vm((rows, chunk), BF16),
        vm((n, rows, chunk), BF16),
        vm((rows, cols), BF16),
        vm((nt, rows, cols), BF16),
        pltpu.SemaphoreType.DMA((len(ops),)),
        pltpu.SemaphoreType.DMA((9, n)),
        pltpu.SemaphoreType.DMA((9, n)),
        pltpu.SemaphoreType.DMA((2, nt)),
        pltpu.SemaphoreType.DMA((2, nt)),
    ]
    return pl.pallas_call(
        functools.partial(step_kernel, n, nt, (rows, cols, heads, span, hidden, cols * n)),
        out_shape=jax.ShapeDtypeStruct((rows, cols), BF16),
        in_specs=[pl.BlockSpec(memory_space=pltpu.SMEM)]
        + [pl.BlockSpec(memory_space=pl.ANY)] * len(ops),
        out_specs=pl.BlockSpec(memory_space=pltpu.VMEM),
        scratch_shapes=scratch,
        compiler_params=pltpu.CompilerParams(
            collective_id=0, has_side_effects=True, vmem_limit_bytes=60 * 1024 * 1024
        ),
    )(lengths, *ops)


def layer(*args):
    tokens, cum_gate, up_weight = args[0], args[9], args[13]
    heads, span = cum_gate.shape[1:]
    if fits(lax.axis_size("kv"), *tokens.shape, heads, span, up_weight.shape[1]):
        return fused(*args)
    return shards(*args)


def solution(mesh):
    return jax.shard_map(
        layer,
        mesh=mesh,
        in_specs=(
            P(None, "kv"),
            P("kv"),
            P("kv", "tp"),
            P("kv", "tp"),
            P("kv", "tp"),
            P(),
            P(),
            P(None, "kv", "tp"),
            P(None, "kv", "tp"),
            P(None, "tp", "kv"),
            P(),
            P("tp", "kv"),
            P("kv"),
            P("kv", "tp"),
            P("tp", "kv"),
        ),
        out_specs=P(None, "kv"),
        check_vma=False,
    )
```
